512 devices in a mesh: fs: 16 (over y, x), tp: 32 (over z, core).
Axes of the slice: x: 4, y: 4, z: 16, core: 2. Of those that a mesh axis runs over, the one named last changes fastest.
Arguments:
- tokens: bfloat16 [8192, 2048], P('fs', 'tp'), may hold values from -6 to 6
- norm_gain: float32 [2048], P('fs'), may hold values from 0.1 to 1.9
- gate_train: float32 [2048, 8192], P('fs', 'tp'), may hold values from -0.125 to 0.125
- up_train: float32 [2048, 8192], P('fs', 'tp'), may hold values from -0.125 to 0.125
- down_train: float32 [8192, 2048], P('fs', 'tp'), may hold values from -0.0625 to 0.0625
Outputs:
- gate_serve: bfloat16 [2048, 8192], P(None, 'tp')
- up_serve: bfloat16 [2048, 8192], P(None, 'tp')
- down_serve: bfloat16 [8192, 2048], P('tp')
- layer_out: bfloat16 [8192, 2048], P(('fs', 'tp'))
The draws below stay inside these ranges and needn't reach their ends.
All inputs are finite; a program needn't handle non-finite values.
Results may differ from the reference program's by a relative error of at most 0.024.
Values may be sent and summed in bfloat16 or wider, within the bound.
No kernel may reach another device: no remote copies, remote signals or barrier semaphores. Data moves between devices by JAX's collectives and lax.ppermute only.
A program may use at most 64 MiB of HBM per device.

```python
import jax
import jax.numpy as jnp
from jax import lax

D = 2048
FF = 8192
TOKENS = 8192


def level_of(own_key, shape, pieces, low, top_value):
    level, own = 1.0, jax.random.fold_in(own_key, 6)
    for position, parts in pieces:
        steps = jnp.exp(jax.random.uniform(jax.random.fold_in(own, position), (parts,), jnp.float32, low / len(pieces), top_value / len(pieces)))
        level = level * jnp.repeat(steps, shape[position] // parts).reshape([-1 if axis == position else 1 for axis in range(len(shape))])
    return level


def centred(own_key, extent, deviation, limit, shards=(), held_as=jnp.bfloat16):
    loudness = level_of(own_key, extent, shards, -0.22, 0.18) if shards else 1.0
    result = jax.random.normal(own_key, extent, jnp.float32) * deviation * loudness
    return jnp.minimum(jnp.maximum(result, -limit), limit).astype(held_as)


def setup_inputs(seed: int = 0) -> dict:
    splits = jax.random.split(jax.random.key(seed), 6)
    tokens = centred(splits[0], (TOKENS, D), 1.0, 6.0, ((0, 16), (1, 32)))
    norm_gain = jnp.clip(1.0 + 0.18 * jax.random.normal(splits[1], (D,), jnp.float32), 0.1, 1.9)
    gate_train = centred(splits[2], (D, FF), D ** -0.5, 0.125, ((0, 16), (1, 32)), jnp.float32)
    up_train = centred(splits[3], (D, FF), D ** -0.5, 0.125, ((0, 16), (1, 32)), jnp.float32)
    down_train = centred(splits[4], (FF, D), FF ** -0.5, 0.0625, ((0, 16), (1, 32)), jnp.float32)
    return dict(tokens=tokens, norm_gain=norm_gain, gate_train=gate_train, up_train=up_train, down_train=down_train)


def reference(tokens, norm_gain, gate_train, up_train, down_train):
    gate_serve = (norm_gain[:, None] * gate_train).astype(jnp.bfloat16)
    up_serve = (norm_gain[:, None] * up_train).astype(jnp.bfloat16)
    down_serve = down_train.astype(jnp.bfloat16)
    wide = tokens.astype(jnp.float32)
    scale = lax.rsqrt(lax.optimization_barrier(jnp.sum(wide * wide, axis=1)) / D + 1e-06)[:, None]
    gate = jnp.dot(tokens, gate_serve, preferred_element_type=jnp.float32)
    up_part = jnp.dot(tokens, up_serve, preferred_element_type=jnp.float32)
    hidden = (jax.nn.silu(gate * scale) * (up_part * scale)).astype(jnp.bfloat16)
    layer_out = jnp.dot(hidden, down_serve, preferred_element_type=jnp.float32).astype(jnp.bfloat16)
    return (gate_serve, up_serve, down_serve, layer_out)
```

```python
import jax
import jax.numpy as jnp
from jax import lax
from jax.sharding import Mesh
from jax.sharding import PartitionSpec as P


D = 2048
PLANE = ("fs",)
Z = ("zh", "zl")
TP = ("zh", "zl", "c")
FS_TP = ("fs", "zh", "zl", "c")
EPS = 1e-06
BF = jnp.bfloat16
F32 = jnp.float32


def pick(x, i, dim):
    return lax.dynamic_index_in_dim(x, i, dim, keepdims=False, allow_negative_indices=False)


def shift(x, by):
    return lax.ppermute(x, Z, [(i, (i + by) % 16) for i in range(16)])


def swap(x):
    return lax.ppermute(x, "c", [(0, 1), (1, 0)])


def spread(x, axis):
    n = lax.axis_size(axis)
    return lax.all_to_all(jnp.broadcast_to(x, (n, *x.shape)), axis, 0, 0, tiled=True)


def gather_tokens(tokens):
    zl, c = lax.axis_index("zl"), lax.axis_index("c")
    own = spread(tokens.T, "zh")
    before, after = shift(own, 1), shift(own, -1)
    far = jnp.concatenate([shift(own[:2], 2), shift(own[2:], -2)], axis=0)
    mine = jnp.stack([before, own, after, far])
    other = swap(mine)
    whole = jnp.zeros((4, 4, 2, 64, 512), BF)
    for s in range(4):
        at = (zl + (s + 3)) & 3
        whole = lax.dynamic_update_slice(whole, mine[s][:, None, None], (0, at, c, 0, 0), allow_negative_indices=False)
        whole = lax.dynamic_update_slice(whole, other[s][:, None, None], (0, at, 1 - c, 0, 0), allow_negative_indices=False)
    return whole.reshape(2048, 512)


def gather_down(down_train):
    piece = down_train.astype(BF).T.reshape(16, 4, 512)
    piece = lax.all_to_all(piece, "fs", 0, 0, tiled=True)
    piece = lax.all_to_all(piece, Z, 0, 0, tiled=True)
    piece = piece.reshape(16, 4, 2, 256).transpose(2, 0, 1, 3)
    piece = lax.all_to_all(piece, "c", 0, 0, tiled=True)
    whole = spread(piece, "fs")
    return whole.transpose(4, 2, 1, 0, 3).reshape(256, 2048)


def scatter_sum(part):
    zl, c = lax.axis_index("zl"), lax.axis_index("c")
    part = part.reshape(4, 4, 2, 16, D)
    keep = pick(part, c, 2)
    give = pick(part, 1 - c, 2)
    pair = (keep.astype(F32) + swap(give).astype(F32)).astype(BF)

    def of(d):
        return pick(pair, (zl + d) & 3, 1)

    ahead, behind, far = of(1), of(3), of(2)
    near = of(0).astype(F32) + shift(ahead, 1).astype(F32) + shift(behind, -1).astype(F32)
    far = jnp.concatenate([shift(far[:2], 2), shift(far[2:], -2)], axis=0)
    near = (near + far.astype(F32)).astype(BF)
    rows = lax.all_to_all(near, "zh", 0, 0, tiled=True)
    return jnp.sum(rows.astype(F32), axis=0).astype(BF)


def body(tokens, norm_gain, gate_train, up_train, down_train):
    gate_local = (norm_gain[:, None] * gate_train).astype(BF)
    up_local = (norm_gain[:, None] * up_train).astype(BF)
    both = spread(jnp.concatenate([gate_local, up_local], axis=1), "fs").reshape(D, 512)
    x = gather_tokens(tokens)
    wide = x.astype(F32)
    scale = lax.rsqrt(jnp.sum(wide * wide, axis=0) / D + EPS)[:, None]
    down = gather_down(down_train)
    sums = lax.dot_general(x, both, (((0,), (0,)), ((), ())), preferred_element_type=F32)
    gate, up = sums[:, :256], sums[:, 256:]
    hidden = (jax.nn.silu(gate * scale) * (up * scale)).astype(BF)
    part = jnp.dot(hidden, down, preferred_element_type=F32).astype(BF)
    return (both[:, :256], both[:, 256:], down, scatter_sum(part))


def solution(mesh):
    finer = Mesh(mesh.devices.reshape(mesh.shape["fs"], 4, 4, 2), FS_TP)
    placed = (P("fs", TP), P("fs"), P("fs", TP), P("fs", TP), P("fs", TP))
    return jax.shard_map(
        body,
        mesh=finer,
        in_specs=placed,
        out_specs=(P(None, TP), P(None, TP), P(TP, None), P(FS_TP, None)),
        check_vma=False,
    )
```

```python
import jax
import jax.numpy as jnp
from jax import lax
from jax.sharding import Mesh
from jax.sharding import PartitionSpec as P


D = 2048
Z = ("zh", "zl")
TP = ("zh", "zl", "c")
FS_TP = ("fs", "zh", "zl", "c")
EPS = 1e-06
BF = jnp.bfloat16
F32 = jnp.float32


def pick(x, i, dim):
    return lax.dynamic_index_in_dim(x, i, dim, keepdims=False, allow_negative_indices=False)


def put(whole, part, at):
    return lax.dynamic_update_slice(whole, part, at, allow_negative_indices=False)


def shift(x, by):
    return lax.ppermute(x, Z, [(i, (i + by) % 16) for i in range(16)])


def swap(x):
    return lax.ppermute(x, "c", [(0, 1), (1, 0)])


def spread(x, axis):
    n = lax.axis_size(axis)
    return lax.all_to_all(jnp.broadcast_to(x, (n, *x.shape)), axis, 0, 0, tiled=True)


def gather_tokens(tokens):
    zh, zl, c = (lax.axis_index(a) for a in TP)
    to = lax.broadcasted_iota(jnp.int32, (512, 512), 1)
    source = ((to >> 4) & 15) * 32 + (to >> 8) * 16 + (to & 15)
    order = (lax.broadcasted_iota(jnp.int32, (512, 512), 0) == source).astype(BF)
    x = jnp.dot(tokens.T, order, preferred_element_type=F32).astype(BF)
    low, high = x[:, :256], x[:, 256:]
    got = swap(jnp.where(c == 0, high, low))
    chip = jnp.concatenate([jnp.where(c == 0, low, got), jnp.where(c == 0, got, high)], axis=0)[None, None]
    own = put(jnp.zeros((4, 1, 128, 256), BF), chip, (zh, 0, 0, 0))
    for by in (1, 3, 2):
        own = put(own, shift(chip, 4 * by), ((zh - by) & 3, 0, 0, 0))
    before, after = shift(own, 1), shift(own, -1)
    far_a, far_b = shift(own[:2], 2), shift(own[2:], -2)
    whole = put(jnp.zeros((4, 4, 128, 256), BF), own, (0, zl, 0, 0))
    whole = put(whole, before, (0, (zl + 3) & 3, 0, 0))
    whole = put(whole, after, (0, (zl + 1) & 3, 0, 0))
    whole = put(whole, far_a, (0, (zl + 2) & 3, 0, 0))
    whole = put(whole, far_b, (2, (zl + 2) & 3, 0, 0))
    return whole.reshape(D, 256)


def gather_down(down_train):
    c = lax.axis_index("c")
    x = down_train.astype(BF).T
    every = [(a, b) for a in range(16) for b in range(16)]
    x = lax.ppermute(x, ("fs", *Z), [(a * 16 + b, (a ^ b) * 16 + b) for a, b in every])
    x = lax.ppermute(x, ("fs", *Z), [((a ^ b) * 16 + b, b * 16 + a) for a, b in every])
    low, high = x[:, :256], x[:, 256:]
    got = swap(jnp.where(c == 0, high, low))
    chip = jnp.concatenate([jnp.where(c == 0, low, got), jnp.where(c == 0, got, high)], axis=0)
    return spread(chip, "fs").reshape(D, 256)


def scatter_sum(part):
    zh, zl = lax.axis_index("zh"), lax.axis_index("zl")
    part = part.reshape(4, 4, 16, D)
    ahead, behind, far = pick(part, (zl + 1) & 3, 1), pick(part, (zl + 3) & 3, 1), pick(part, (zl + 2) & 3, 1)
    near = pick(part, zl, 1).astype(F32)
    near += shift(ahead, 1).astype(F32) + shift(behind, -1).astype(F32)
    far = jnp.concatenate([shift(far[:2], 2), shift(far[2:], -2)], axis=0)
    near += far.astype(F32)
    total = pick(near, zh, 0)
    low = near.astype(BF)
    for by in (1, 3, 2):
        total += shift(pick(low, (zh + by) & 3, 0), 4 * by).astype(F32)
    return total.astype(BF)


def hidden_of(x, scale, both):
    sums = lax.dot_general(x, both, (((0,), (0,)), ((), ())), preferred_element_type=F32)
    gate, up = sums[:, :256], sums[:, 256:]
    return (jax.nn.silu(gate * scale) * (up * scale)).astype(BF)


def body(tokens, norm_gain, gate_train, up_train, down_train):
    gate_local = (norm_gain[:, None] * gate_train).astype(BF)
    up_local = (norm_gain[:, None] * up_train).astype(BF)
    both = spread(jnp.concatenate([gate_local, up_local], axis=1), "fs").reshape(D, 512)
    x = gather_tokens(tokens)
    wide = x.astype(F32)
    scale = lax.rsqrt(jnp.sum(wide * wide, axis=0) / D + EPS)[:, None]
    down = gather_down(down_train)
    other_both = swap(both)
    other_down = swap(down)
    mine, others = hidden_of(x, scale, both), hidden_of(x, scale, other_both)
    across = (((1,), (1,)), ((), ()))
    part = lax.dot_general(mine, down, across, preferred_element_type=F32)
    part += lax.dot_general(others, other_down, across, preferred_element_type=F32)
    return (both[:, :256], both[:, 256:], down.T, scatter_sum(part.astype(BF)))


def solution(mesh):
    finer = Mesh(mesh.devices.reshape(mesh.shape["fs"], 4, 4, 2), FS_TP)
    placed = (P("fs", TP), P("fs"), P("fs", TP), P("fs", TP), P("fs", TP))
    return jax.shard_map(
        body,
        mesh=finer,
        in_specs=placed,
        out_specs=(P(None, TP), P(None, TP), P(TP, None), P(FS_TP, None)),
        check_vma=False,
    )
```

```python
import jax
import jax.numpy as jnp
from jax import lax
from jax.sharding import Mesh
from jax.sharding import PartitionSpec as P


D = 2048
TP = ("zh", "zl", "c")
FS_TP = ("fs", "zh", "zl", "c")
EPS = 1e-06
BF = jnp.bfloat16
F32 = jnp.float32
EVERY = [(a, b) for a in range(16) for b in range(16)]


def pick(x, i, dim):
    return lax.dynamic_index_in_dim(x, i, dim, keepdims=False, allow_negative_indices=False)


def part_of(x, at, size, dim):
    return lax.dynamic_slice_in_dim(x, at, size, dim, allow_negative_indices=False)


def put(whole, part, at):
    return lax.dynamic_update_slice(whole, part, at, allow_negative_indices=False)


def shift(x, by):
    return lax.ppermute(x, TP[:2], [(i, (i + by) % 16) for i in range(16)])


def fan(x, by):
    pairs = [(2 * z + c, 2 * ((z + (by, -by)[c]) % 16) + c) for z in range(16) for c in range(2)]
    return lax.ppermute(x, TP, pairs)


def swap(x):
    return lax.ppermute(x, "c", [(0, 1), (1, 0)])


def by_core(c, mine, other, dim):
    return jnp.concatenate([jnp.where(c == 0, mine, other), jnp.where(c == 0, other, mine)], axis=dim)


def gather_tokens(tokens):
    zh, zl, c = (lax.axis_index(a) for a in TP)
    x = tokens.T
    chip = by_core(c, x, swap(x), 0)
    p = fan(chip, 4)
    q = fan(jnp.where(c == 0, chip[:, :256], chip[:, 256:]), 8)
    o = swap(jnp.concatenate([p, q], axis=1))
    own = put(jnp.zeros((4, 128, 512), BF), chip[None], (zh, 0, 0))
    own = put(own, p[None], ((zh + 3 + 2 * c) & 3, 0, 0))
    own = put(own, o[None, :, :512], ((zh + 1 + 2 * c) & 3, 0, 0))
    own = put(own, by_core(c, q, o[:, 512:], 1)[None], ((zh + 2) & 3, 0, 0))
    n = fan(own, 1)
    f = fan(part_of(own, 2 * c, 2, 0), 2)
    o = swap(jnp.concatenate([n, f], axis=0))
    whole = put(jnp.zeros((4, 4, 128, 512), BF), own[:, None], (0, zl, 0, 0))
    whole = put(whole, n[:, None], (0, (zl + 3 + 2 * c) & 3, 0, 0))
    whole = put(whole, f[:, None], (2 * c, (zl + 2) & 3, 0, 0))
    whole = put(whole, o[:4, None], (0, (zl + 1 + 2 * c) & 3, 0, 0))
    whole = put(whole, o[4:, None], (2 - 2 * c, (zl + 2) & 3, 0, 0))
    return whole.reshape(D, 512)


def place_down(down_train):
    c = lax.axis_index("c")
    x = down_train.astype(BF).T
    x = lax.ppermute(x, FS_TP[:3], [(a * 16 + b, (a ^ b) * 16 + b) for a, b in EVERY])
    x = lax.ppermute(x, FS_TP[:3], [((a ^ b) * 16 + b, b * 16 + a) for a, b in EVERY])
    keep, give = jnp.where(c == 0, x[:, :256], x[:, 256:]), jnp.where(c == 0, x[:, 256:], x[:, :256])
    return by_core(c, keep, swap(give), 0)


def scatter_sum(hidden, down):
    _, zl, c = (lax.axis_index(a) for a in TP)
    hidden = hidden.reshape(16, 2, 16, 256)
    across = (((1,), (1,)), ((), ()))
    keep, give = pick(hidden, c, 1).reshape(256, 256), pick(hidden, 1 - c, 1).reshape(256, 256)
    give = lax.dot_general(give, down, across, preferred_element_type=F32).astype(BF)
    got = swap(give)
    pair = lax.dot_general(keep, down, across, preferred_element_type=F32) + got.astype(F32)
    pair = pair.astype(BF).reshape(4, 4, 16, D)
    ahead, behind, far = (pick(pair, (zl + d) & 3, 1) for d in (1, 3, 2))
    near = pick(pair, zl, 1).astype(F32)
    near += shift(ahead, 1).astype(F32) + shift(behind, -1).astype(F32)
    far = jnp.concatenate([shift(far[:2], 2), shift(far[2:], -2)], axis=0)
    near = (near + far.astype(F32)).astype(BF)
    rows = lax.all_to_all(near, "zh", 0, 0, tiled=True)
    return jnp.sum(rows.astype(F32), axis=0).astype(BF)


def body(tokens, norm_gain, gate_train, up_train, down_train):
    gate_local = (norm_gain[:, None] * gate_train).astype(BF)
    up_local = (norm_gain[:, None] * up_train).astype(BF)
    local = jnp.concatenate([gate_local, up_local, place_down(down_train)], axis=1)
    every = lax.all_to_all(jnp.broadcast_to(local, (16, 128, 768)), "fs", 0, 0, tiled=True)
    every = every.reshape(D, 768)
    both, down = every[:, :512], every[:, 512:]
    x = gather_tokens(tokens)
    wide = x.astype(F32)
    scale = lax.rsqrt(jnp.sum(wide * wide, axis=0) / D + EPS)[:, None]
    sums = lax.dot_general(x, both, (((0,), (0,)), ((), ())), preferred_element_type=F32)
    gate, up = sums[:, :256], sums[:, 256:]
    hidden = (jax.nn.silu(gate * scale) * (up * scale)).astype(BF)
    return (both[:, :256], both[:, 256:], down.T, scatter_sum(hidden, down))


def solution(mesh):
    finer = Mesh(mesh.devices.reshape(mesh.shape["fs"], 4, 4, 2), FS_TP)
    placed = (P("fs", TP), P("fs"), P("fs", TP), P("fs", TP), P("fs", TP))
    return jax.shard_map(
        body,
        mesh=finer,
        in_specs=placed,
        out_specs=(P(None, TP), P(None, TP), P(TP, None), P(FS_TP, None)),
        check_vma=False,
    )
```

```python
import jax
import jax.numpy as jnp
from jax import lax
from jax.experimental.layout import Layout, with_layout_constraint
from jax.sharding import Mesh
from jax.sharding import PartitionSpec as P


D = 2048
TP = ("zh", "zl", "c")
FS_TP = ("fs", "zh", "zl", "c")
EPS = 1e-06
BF = jnp.bfloat16
F32 = jnp.float32
EVERY = [(a, b) for a in range(16) for b in range(16)]


def pick(x, i, dim):
    return lax.dynamic_index_in_dim(x, i, dim, keepdims=False, allow_negative_indices=False)


def put(whole, part, at):
    return lax.dynamic_update_slice(whole, part, at, allow_negative_indices=False)


def shift(x, by):
    return lax.ppermute(x, TP[:2], [(i, (i + by) % 16) for i in range(16)])


def swap(x):
    return lax.ppermute(x, "c", [(0, 1), (1, 0)])


def by_core(c, mine, other, dim):
    return jnp.concatenate([jnp.where(c == 0, mine, other), jnp.where(c == 0, other, mine)], axis=dim)


def row_major(x):
    return with_layout_constraint(x, Layout(major_to_minor=tuple(range(x.ndim))))


def gather_tokens(tokens):
    zl, c = lax.axis_index("zl"), lax.axis_index("c")
    own = lax.all_to_all(jnp.broadcast_to(tokens.T, (4, 64, 512)), "zh", 0, 0, tiled=True)
    before, after = shift(own, 1), shift(own, -1)
    far_a, far_b = shift(own[:2], 2), shift(own[2:], -2)
    mine = put(jnp.zeros((4, 4, 64, 512), BF), own[:, None], (0, zl, 0, 0))
    mine = put(mine, before[:, None], (0, (zl + 3) & 3, 0, 0))
    mine = put(mine, after[:, None], (0, (zl + 1) & 3, 0, 0))
    mine = put(mine, far_a[:, None], (0, (zl + 2) & 3, 0, 0))
    mine = put(mine, far_b[:, None], (2, (zl + 2) & 3, 0, 0)).reshape(16, 1, 64, 512)
    other = swap(mine)
    whole = put(jnp.zeros((16, 2, 64, 512), BF), mine, (0, c, 0, 0))
    return put(whole, other, (0, 1 - c, 0, 0)).reshape(D, 512)


def place_down(down_train):
    c = lax.axis_index("c")
    x = down_train.astype(BF).T
    x = lax.ppermute(x, FS_TP[:3], [(a * 16 + b, (a ^ b) * 16 + b) for a, b in EVERY])
    x = lax.ppermute(x, FS_TP[:3], [((a ^ b) * 16 + b, b * 16 + a) for a, b in EVERY])
    keep, give = jnp.where(c == 0, x[:, :256], x[:, 256:]), jnp.where(c == 0, x[:, 256:], x[:, :256])
    return by_core(c, keep, swap(give), 0)


def scatter_sum(hidden, down):
    _, zl, c = (lax.axis_index(a) for a in TP)
    hidden = hidden.reshape(16, 2, 16, 256)
    across = (((1,), (1,)), ((), ()))
    keep, give = pick(hidden, c, 1).reshape(256, 256), pick(hidden, 1 - c, 1).reshape(256, 256)
    give = lax.dot_general(give, down, across, preferred_element_type=F32).astype(BF)
    got = swap(give)
    pair = lax.dot_general(keep, down, across, preferred_element_type=F32) + got.astype(F32)
    pair = pair.astype(BF).reshape(4, 4, 16, D)
    ahead, behind, far = (pick(pair, (zl + d) & 3, 1) for d in (1, 3, 2))
    near = pick(pair, zl, 1).astype(F32)
    near += shift(ahead, 1).astype(F32) + shift(behind, -1).astype(F32)
    far = jnp.concatenate([shift(far[:2], 2), shift(far[2:], -2)], axis=0)
    near = (near + far.astype(F32)).astype(BF)
    rows = lax.all_to_all(near, "zh", 0, 0, tiled=True)
    return jnp.sum(rows.astype(F32), axis=0).astype(BF)


def body(tokens, norm_gain, gate_train, up_train, down_train):
    gate_local = (norm_gain[:, None] * gate_train).astype(BF)
    up_local = (norm_gain[:, None] * up_train).astype(BF)
    local = jnp.concatenate([gate_local, up_local, place_down(down_train)], axis=1)
    every = row_major(jnp.broadcast_to(local, (16, 128, 768)))
    every = row_major(lax.all_to_all(every, "fs", 0, 0, tiled=True))
    every = every.reshape(D, 768)
    both, down = every[:, :512], every[:, 512:]
    x = gather_tokens(tokens)
    wide = x.astype(F32)
    scale = lax.rsqrt(jnp.sum(wide * wide, axis=0) / D + EPS)[:, None]
    sums = lax.dot_general(x, both, (((0,), (0,)), ((), ())), preferred_element_type=F32)
    gate, up = sums[:, :256], sums[:, 256:]
    hidden = (jax.nn.silu(gate * scale) * (up * scale)).astype(BF)
    return (both[:, :256], both[:, 256:], down.T, scatter_sum(hidden, down))


def solution(mesh):
    finer = Mesh(mesh.devices.reshape(mesh.shape["fs"], 4, 4, 2), FS_TP)
    placed = (P("fs", TP), P("fs"), P("fs", TP), P("fs", TP), P("fs", TP))
    return jax.shard_map(
        body,
        mesh=finer,
        in_specs=placed,
        out_specs=(P(None, TP), P(None, TP), P(TP, None), P(FS_TP, None)),
        check_vma=False,
    )
```

```python
import jax
import jax.numpy as jnp
from jax import lax
from jax.experimental.layout import Layout, with_layout_constraint
from jax.sharding import Mesh
from jax.sharding import PartitionSpec as P


D = 2048
TP = ("zh", "zl", "c")
FS_TP = ("fs", "zh", "zl", "c")
EPS = 1e-06
BF = jnp.bfloat16
F32 = jnp.float32
EVERY = [(a, b) for a in range(16) for b in range(16)]


def pick(x, i, dim):
    return lax.dynamic_index_in_dim(x, i, dim, keepdims=False, allow_negative_indices=False)


def part_of(x, at, size, dim):
    return lax.dynamic_slice_in_dim(x, at, size, dim, allow_negative_indices=False)


def put(whole, part, at):
    return lax.dynamic_update_slice(whole, part, at, allow_negative_indices=False)


def shift(x, by):
    return lax.ppermute(x, TP[:2], [(i, (i + by) % 16) for i in range(16)])


def fan(x, by):
    pairs = [(2 * z + c, 2 * ((z + (by, -by)[c]) % 16) + c) for z in range(16) for c in range(2)]
    return lax.ppermute(x, TP, pairs)


def swap(x):
    return lax.ppermute(x, "c", [(0, 1), (1, 0)])


def by_core(c, mine, other, dim):
    return jnp.concatenate([jnp.where(c == 0, mine, other), jnp.where(c == 0, other, mine)], axis=dim)


def row_major(x):
    return with_layout_constraint(x, Layout(major_to_minor=tuple(range(x.ndim))))


def spread(x):
    every = row_major(jnp.broadcast_to(x, (16, *x.shape)))
    return row_major(lax.all_to_all(every, "fs", 0, 0, tiled=True)).reshape(D, x.shape[1])


def gather_tokens(tokens):
    zh, zl, c = (lax.axis_index(a) for a in TP)
    x = tokens.T
    chip = by_core(c, x, swap(x), 0)
    p = fan(chip, 4)
    q = fan(jnp.where(c == 0, chip[:, :256], chip[:, 256:]), 8)
    o = swap(jnp.concatenate([p, q], axis=1))
    own = put(jnp.zeros((4, 128, 512), BF), chip[None], (zh, 0, 0))
    own = put(own, p[None], ((zh + 3 + 2 * c) & 3, 0, 0))
    own = put(own, o[None, :, :512], ((zh + 1 + 2 * c) & 3, 0, 0))
    own = put(own, by_core(c, q, o[:, 512:], 1)[None], ((zh + 2) & 3, 0, 0))
    n = fan(own, 1)
    f = fan(part_of(own, 2 * c, 2, 0), 2)
    o = swap(jnp.concatenate([n, f], axis=0))
    whole = put(jnp.zeros((4, 4, 128, 512), BF), own[:, None], (0, zl, 0, 0))
    whole = put(whole, n[:, None], (0, (zl + 3 + 2 * c) & 3, 0, 0))
    whole = put(whole, f[:, None], (2 * c, (zl + 2) & 3, 0, 0))
    whole = put(whole, o[:4, None], (0, (zl + 1 + 2 * c) & 3, 0, 0))
    whole = put(whole, o[4:, None], (2 - 2 * c, (zl + 2) & 3, 0, 0))
    return whole.reshape(D, 512)


def place_down(down_train):
    c = lax.axis_index("c")
    x = down_train.astype(BF).T
    x = lax.ppermute(x, FS_TP[:3], [(a * 16 + b, (a ^ b) * 16 + b) for a, b in EVERY])
    x = lax.ppermute(x, FS_TP[:3], [((a ^ b) * 16 + b, b * 16 + a) for a, b in EVERY])
    keep, give = jnp.where(c == 0, x[:, :256], x[:, 256:]), jnp.where(c == 0, x[:, 256:], x[:, :256])
    return by_core(c, keep, swap(give), 0)


def scatter_sum(hidden, down, ready):
    _, zl, c = (lax.axis_index(a) for a in TP)
    hidden = hidden.reshape(16, 2, 16, 256)
    across = (((1,), (1,)), ((), ()))
    keep, give = pick(hidden, c, 1).reshape(256, 256), pick(hidden, 1 - c, 1).reshape(256, 256)
    give = lax.dot_general(give, down, across, preferred_element_type=F32).astype(BF)
    got = swap(give)
    pair = lax.dot_general(keep, down, across, preferred_element_type=F32) + got.astype(F32)
    pair = pair.astype(BF).reshape(4, 4, 16, D)
    ahead, behind, far = (pick(pair, (zl + d) & 3, 1) for d in (1, 3, 2))
    near = pick(pair, zl, 1).astype(F32)
    near += shift(ahead, 1).astype(F32) + shift(behind, -1).astype(F32)
    far = jnp.concatenate([shift(far[:2], 2), shift(far[2:], -2)], axis=0)
    near, ready = lax.optimization_barrier(((near + far.astype(F32)).astype(BF), ready))
    rows = lax.all_to_all(near, "zh", 0, 0, tiled=True)
    return (*ready, jnp.sum(rows.astype(F32), axis=0).astype(BF))


def body(tokens, norm_gain, gate_train, up_train, down_train):
    gate_local = (norm_gain[:, None] * gate_train).astype(BF)
    up_local = (norm_gain[:, None] * up_train).astype(BF)
    both = spread(jnp.concatenate([gate_local, up_local], axis=1))
    down = spread(place_down(down_train))
    x = gather_tokens(tokens)
    wide = x.astype(F32)
    scale = lax.rsqrt(jnp.sum(wide * wide, axis=0) / D + EPS)[:, None]
    sums = lax.dot_general(x, both, (((0,), (0,)), ((), ())), preferred_element_type=F32)
    gate, up = sums[:, :256], sums[:, 256:]
    hidden = (jax.nn.silu(gate * scale) * (up * scale)).astype(BF)
    return scatter_sum(hidden, down, (both[:, :256], both[:, 256:], down.T))


def solution(mesh):
    finer = Mesh(mesh.devices.reshape(mesh.shape["fs"], 4, 4, 2), FS_TP)
    placed = (P("fs", TP), P("fs"), P("fs", TP), P("fs", TP), P("fs", TP))
    return jax.shard_map(
        body,
        mesh=finer,
        in_specs=placed,
        out_specs=(P(None, TP), P(None, TP), P(TP, None), P(FS_TP, None)),
        check_vma=False,
    )
```

```python
import jax
import jax.numpy as jnp
from jax import lax
from jax.experimental.layout import Layout, with_layout_constraint
from jax.sharding import Mesh
from jax.sharding import PartitionSpec as P


D = 2048
TP = ("zh", "zl", "c")
FS_TP = ("fs", "zh", "zl", "c")
EPS = 1e-06
SCALE = 8192.0
BF = jnp.bfloat16
F32 = jnp.float32
EVERY = [(a, b) for a in range(16) for b in range(16)]


def pick(x, i, dim):
    return lax.dynamic_index_in_dim(x, i, dim, keepdims=False, allow_negative_indices=False)


def put(whole, part, at):
    return lax.dynamic_update_slice(whole, part, at, allow_negative_indices=False)


def shift(x, by):
    return lax.ppermute(x, TP[:2], [(i, (i + by) % 16) for i in range(16)])


def swap(x):
    return lax.ppermute(x, "c", [(0, 1), (1, 0)])


def by_core(c, mine, other, dim):
    return jnp.concatenate([jnp.where(c == 0, mine, other), jnp.where(c == 0, other, mine)], axis=dim)


def row_major(x):
    return with_layout_constraint(x, Layout(major_to_minor=tuple(range(x.ndim))))


def spread(x):
    every = row_major(jnp.broadcast_to(x, (16, *x.shape)))
    return row_major(lax.all_to_all(every, "fs", 0, 0, tiled=True)).reshape(D, x.shape[1])


def gather_tokens(tokens):
    c = lax.axis_index("c")
    x = (tokens.T.astype(F32) * SCALE).astype(jnp.float16)
    mine = lax.all_gather(x, TP[:2])[:, None]
    other = swap(mine)
    mine, other = ((v.astype(F32) / SCALE).astype(BF) for v in (mine, other))
    whole = put(jnp.zeros((16, 2, 64, 512), BF), mine, (0, c, 0, 0))
    return put(whole, other, (0, 1 - c, 0, 0)).reshape(D, 512)


def place_down(down_train):
    c = lax.axis_index("c")
    x = down_train.astype(BF).T
    x = lax.ppermute(x, FS_TP[:3], [(a * 16 + b, (a ^ b) * 16 + b) for a, b in EVERY])
    x = lax.ppermute(x, FS_TP[:3], [((a ^ b) * 16 + b, b * 16 + a) for a, b in EVERY])
    keep, give = jnp.where(c == 0, x[:, :256], x[:, 256:]), jnp.where(c == 0, x[:, 256:], x[:, :256])
    return by_core(c, keep, swap(give), 0)


def scatter_sum(hidden, down, ready):
    _, zl, c = (lax.axis_index(a) for a in TP)
    hidden = hidden.reshape(16, 2, 16, 256)
    across = (((1,), (1,)), ((), ()))
    keep, give = pick(hidden, c, 1).reshape(256, 256), pick(hidden, 1 - c, 1).reshape(256, 256)
    give = lax.dot_general(give, down, across, preferred_element_type=F32).astype(BF)
    got = swap(give)
    pair = lax.dot_general(keep, down, across, preferred_element_type=F32) + got.astype(F32)
    pair = pair.astype(BF).reshape(4, 4, 16, D)
    ahead, behind, far = (pick(pair, (zl + d) & 3, 1) for d in (1, 3, 2))
    near = pick(pair, zl, 1).astype(F32)
    near += shift(ahead, 1).astype(F32) + shift(behind, -1).astype(F32)
    far = jnp.concatenate([shift(far[:2], 2), shift(far[2:], -2)], axis=0)
    near, ready = lax.optimization_barrier(((near + far.astype(F32)).astype(BF), ready))
    rows = lax.all_to_all(near, "zh", 0, 0, tiled=True)
    return (*ready, jnp.sum(rows.astype(F32), axis=0).astype(BF))


def body(tokens, norm_gain, gate_train, up_train, down_train):
    gate_local = (norm_gain[:, None] * gate_train).astype(BF)
    up_local = (norm_gain[:, None] * up_train).astype(BF)
    both = spread(jnp.concatenate([gate_local, up_local], axis=1))
    down = spread(place_down(down_train))
    x = gather_tokens(tokens)
    wide = x.astype(F32)
    scale = lax.rsqrt(jnp.sum(wide * wide, axis=0) / D + EPS)[:, None]
    sums = lax.dot_general(x, both, (((0,), (0,)), ((), ())), preferred_element_type=F32)
    gate, up = sums[:, :256], sums[:, 256:]
    hidden = (jax.nn.silu(gate * scale) * (up * scale)).astype(BF)
    return scatter_sum(hidden, down, (both[:, :256], both[:, 256:], down.T))


def solution(mesh):
    finer = Mesh(mesh.devices.reshape(mesh.shape["fs"], 4, 4, 2), FS_TP)
    placed = (P("fs", TP), P("fs"), P("fs", TP), P("fs", TP), P("fs", TP))
    return jax.shard_map(
        body,
        mesh=finer,
        in_specs=placed,
        out_specs=(P(None, TP), P(None, TP), P(TP, None), P(FS_TP, None)),
        check_vma=False,
    )
```

```python
import jax
import jax.numpy as jnp
from jax import lax
from jax.experimental.layout import Layout, with_layout_constraint
from jax.sharding import Mesh
from jax.sharding import PartitionSpec as P


D = 2048
TP = ("zh", "zl", "c")
FS_TP = ("fs", "zh", "zl", "c")
EPS = 1e-06
SCALE = 8192.0
BF = jnp.bfloat16
F32 = jnp.float32
EVERY = [(a, b) for a in range(16) for b in range(16)]


def pick(x, i, dim):
    return lax.dynamic_index_in_dim(x, i, dim, keepdims=False, allow_negative_indices=False)


def put(whole, part, at):
    return lax.dynamic_update_slice(whole, part, at, allow_negative_indices=False)


def shift(x, by):
    return lax.ppermute(x, TP[:2], [(i, (i + by) % 16) for i in range(16)])


def swap(x):
    return lax.ppermute(x, "c", [(0, 1), (1, 0)])


def by_core(c, mine, other, dim):
    return jnp.concatenate([jnp.where(c == 0, mine, other), jnp.where(c == 0, other, mine)], axis=dim)


def row_major(x):
    return with_layout_constraint(x, Layout(major_to_minor=tuple(range(x.ndim))))


def gather_tokens(tokens):
    c = lax.axis_index("c")
    x = (tokens.T.astype(F32) * SCALE).astype(jnp.float16)
    mine = lax.all_gather(x, TP[:2])[:, None]
    other = swap(mine)
    mine, other = ((v.astype(F32) / SCALE).astype(BF) for v in (mine, other))
    whole = put(jnp.zeros((16, 2, 64, 512), BF), mine, (0, c, 0, 0))
    return put(whole, other, (0, 1 - c, 0, 0)).reshape(D, 512)


def place_down(down_train):
    c = lax.axis_index("c")
    x = down_train.astype(BF).T
    keep, give = jnp.where(c == 0, x[:, :256], x[:, 256:]), jnp.where(c == 0, x[:, 256:], x[:, :256])
    x = by_core(c, keep, swap(give), 0)
    x = lax.ppermute(x, FS_TP[:3], [(a * 16 + b, (a ^ b) * 16 + b) for a, b in EVERY])
    return lax.ppermute(x, FS_TP[:3], [((a ^ b) * 16 + b, b * 16 + a) for a, b in EVERY])


def scatter_sum(hidden, down, ready):
    _, zl, c = (lax.axis_index(a) for a in TP)
    hidden = hidden.reshape(16, 2, 16, 256)
    across = (((1,), (1,)), ((), ()))
    keep, give = pick(hidden, c, 1).reshape(256, 256), pick(hidden, 1 - c, 1).reshape(256, 256)
    give = lax.dot_general(give, down, across, preferred_element_type=F32).astype(BF)
    got = swap(give)
    pair = lax.dot_general(keep, down, across, preferred_element_type=F32) + got.astype(F32)
    pair = pair.astype(BF).reshape(4, 4, 16, D)
    ahead, behind, far = (pick(pair, (zl + d) & 3, 1) for d in (1, 3, 2))
    near = pick(pair, zl, 1).astype(F32)
    near += shift(ahead, 1).astype(F32) + shift(behind, -1).astype(F32)
    far = jnp.concatenate([shift(far[:2], 2), shift(far[2:], -2)], axis=0)
    near, ready = lax.optimization_barrier(((near + far.astype(F32)).astype(BF), ready))
    rows = lax.all_to_all(near, "zh", 0, 0, tiled=True)
    return (*ready, jnp.sum(rows.astype(F32), axis=0).astype(BF))


def body(tokens, norm_gain, gate_train, up_train, down_train):
    gate_local = (norm_gain[:, None] * gate_train).astype(BF)
    up_local = (norm_gain[:, None] * up_train).astype(BF)
    local = jnp.concatenate([gate_local, up_local, jnp.zeros((128, 256), BF)], axis=1)
    every = lax.optimization_barrier(row_major(jnp.broadcast_to(local, (16, 128, 768))))
    down = jnp.broadcast_to(place_down(down_train), (16, 128, 256))
    every = lax.dynamic_update_slice(every, down, (0, 0, 512))
    every = row_major(lax.all_to_all(every, "fs", 0, 0, tiled=True)).reshape(D, 768)
    both, down = every[:, :512], every[:, 512:]
    x = gather_tokens(tokens)
    wide = x.astype(F32)
    scale = lax.rsqrt(jnp.sum(wide * wide, axis=0) / D + EPS)[:, None]
    sums = lax.dot_general(x, both, (((0,), (0,)), ((), ())), preferred_element_type=F32)
    gate, up = sums[:, :256], sums[:, 256:]
    hidden = (jax.nn.silu(gate * scale) * (up * scale)).astype(BF)
    return scatter_sum(hidden, down, (both[:, :256], both[:, 256:], down.T))


def solution(mesh):
    finer = Mesh(mesh.devices.reshape(mesh.shape["fs"], 4, 4, 2), FS_TP)
    placed = (P("fs", TP), P("fs"), P("fs", TP), P("fs", TP), P("fs", TP))
    return jax.shard_map(
        body,
        mesh=finer,
        in_specs=placed,
        out_specs=(P(None, TP), P(None, TP), P(TP, None), P(FS_TP, None)),
        check_vma=False,
    )
```

```python
import jax
import jax.numpy as jnp
from jax import lax
from jax.experimental.layout import Layout, with_layout_constraint
from jax.sharding import Mesh
from jax.sharding import PartitionSpec as P


D = 2048
TP = ("zh", "zl", "c")
FS_TP = ("fs", "zh", "zl", "c")
EPS = 1e-06
SCALE = 8192.0
BF = jnp.bfloat16
F32 = jnp.float32
EVERY = [(a, b) for a in range(16) for b in range(16)]


def pick(x, i, dim):
    return lax.dynamic_index_in_dim(x, i, dim, keepdims=False, allow_negative_indices=False)


def put(whole, part, at):
    return lax.dynamic_update_slice(whole, part, at, allow_negative_indices=False)


def shift(x, by):
    return lax.ppermute(x, TP[:2], [(i, (i + by) % 16) for i in range(16)])


def swap(x):
    return lax.ppermute(x, "c", [(0, 1), (1, 0)])


def by_core(c, mine, other, dim):
    return jnp.concatenate([jnp.where(c == 0, mine, other), jnp.where(c == 0, other, mine)], axis=dim)


def row_major(x):
    return with_layout_constraint(x, Layout(major_to_minor=tuple(range(x.ndim))))


def spread(x):
    every = row_major(jnp.broadcast_to(x, (16, *x.shape)))
    return row_major(lax.all_to_all(every, "fs", 0, 0, tiled=True)).reshape(D, x.shape[1])


def gather_tokens(tokens):
    c = lax.axis_index("c")
    x = (tokens.T.astype(F32) * SCALE).astype(jnp.float16)
    mine = lax.all_gather(x, TP[:2])[:, None]
    other = swap(mine)
    mine, other = ((v.astype(F32) / SCALE).astype(BF) for v in (mine, other))
    whole = put(jnp.zeros((16, 2, 64, 512), BF), mine, (0, c, 0, 0))
    return put(whole, other, (0, 1 - c, 0, 0)).reshape(D, 512)


def place_down(down_train):
    c = lax.axis_index("c")
    x = down_train.astype(BF).T
    keep, give = jnp.where(c == 0, x[:, :256], x[:, 256:]), jnp.where(c == 0, x[:, 256:], x[:, :256])
    x = by_core(c, keep, swap(give), 0)
    x = lax.ppermute(x, FS_TP[:3], [(a * 16 + b, (a ^ b) * 16 + b) for a, b in EVERY])
    return lax.ppermute(x, FS_TP[:3], [((a ^ b) * 16 + b, b * 16 + a) for a, b in EVERY])


def scatter_sum(hidden, down, ready):
    _, zl, c = (lax.axis_index(a) for a in TP)
    hidden = hidden.reshape(16, 2, 16, 256)
    across = (((1,), (1,)), ((), ()))
    keep, give = pick(hidden, c, 1).reshape(256, 256), pick(hidden, 1 - c, 1).reshape(256, 256)
    give = lax.dot_general(give, down, across, preferred_element_type=F32).astype(BF)
    got = swap(give)
    pair = lax.dot_general(keep, down, across, preferred_element_type=F32) + got.astype(F32)
    pair = pair.astype(BF).reshape(4, 4, 16, D)
    ahead, behind, far = (pick(pair, (zl + d) & 3, 1) for d in (1, 3, 2))
    near = pick(pair, zl, 1).astype(F32)
    near += shift(ahead, 1).astype(F32) + shift(behind, -1).astype(F32)
    far = jnp.concatenate([shift(far[:2], 2), shift(far[2:], -2)], axis=0)
    near, ready = lax.optimization_barrier(((near + far.astype(F32)).astype(BF), ready))
    rows = lax.all_to_all(near, "zh", 0, 0, tiled=True)
    return (*ready, jnp.sum(rows.astype(F32), axis=0).astype(BF))


def body(tokens, norm_gain, gate_train, up_train, down_train):
    gate_local = (norm_gain[:, None] * gate_train).astype(BF)
    up_local = (norm_gain[:, None] * up_train).astype(BF)
    both = spread(jnp.concatenate([gate_local, up_local], axis=1))
    down = spread(place_down(down_train))
    x = gather_tokens(tokens)
    wide = x.astype(F32)
    scale = lax.rsqrt(jnp.sum(wide * wide, axis=0) / D + EPS)[:, None]
    sums = lax.dot_general(x, both, (((0,), (0,)), ((), ())), preferred_element_type=F32)
    gate, up = sums[:, :256], sums[:, 256:]
    hidden = (jax.nn.silu(gate * scale) * (up * scale)).astype(BF)
    gate_serve, up_serve = both[:, :256], both[:, 256:]
    return scatter_sum(hidden, down, (gate_serve, up_serve, down.T))


def solution(mesh):
    finer = Mesh(mesh.devices.reshape(mesh.shape["fs"], 4, 4, 2), FS_TP)
    placed = (P("fs", TP), P("fs"), P("fs", TP), P("fs", TP), P("fs", TP))
    return jax.shard_map(
        body,
        mesh=finer,
        in_specs=placed,
        out_specs=(P(None, TP), P(None, TP), P(TP, None), P(FS_TP, None)),
        check_vma=False,
    )
```

```python
import jax
import jax.numpy as jnp
from jax import lax
from jax.experimental.layout import Layout, with_layout_constraint
from jax.sharding import Mesh
from jax.sharding import PartitionSpec as P


D = 2048
TP = ("zh", "zl", "c")
FS_TP = ("fs", "zh", "zl", "c")
EPS = 1e-06
SCALE = 8192.0
BF = jnp.bfloat16
F32 = jnp.float32
EVERY = [(a, b) for a in range(16) for b in range(16)]


def pick(x, i, dim):
    return lax.dynamic_index_in_dim(x, i, dim, keepdims=False, allow_negative_indices=False)


def part_of(x, at, size, dim):
    return lax.dynamic_slice_in_dim(x, at, size, dim, allow_negative_indices=False)


def put(whole, part, at):
    return lax.dynamic_update_slice(whole, part, at, allow_negative_indices=False)


def fan(x, by):
    pairs = [(2 * z + c, 2 * ((z + (by, -by)[c]) % 16) + c) for z in range(16) for c in range(2)]
    return lax.ppermute(x, TP, pairs)


def swap(x):
    return lax.ppermute(x, "c", [(0, 1), (1, 0)])


def by_core(c, mine, other, dim):
    return jnp.concatenate([jnp.where(c == 0, mine, other), jnp.where(c == 0, other, mine)], axis=dim)


def row_major(x):
    return with_layout_constraint(x, Layout(major_to_minor=tuple(range(x.ndim))))


def spread(x):
    every = row_major(jnp.broadcast_to(x, (16, *x.shape)))
    return row_major(lax.all_to_all(every, "fs", 0, 0, tiled=True)).reshape(D, x.shape[1])


def gather_tokens(tokens):
    c = lax.axis_index("c")
    x = (tokens.T.astype(F32) * SCALE).astype(jnp.float16)
    mine = lax.all_gather(x, TP[:2])[:, None]
    other = swap(mine)
    mine, other = ((v.astype(F32) / SCALE).astype(BF) for v in (mine, other))
    whole = put(jnp.zeros((16, 2, 64, 512), BF), mine, (0, c, 0, 0))
    return put(whole, other, (0, 1 - c, 0, 0)).reshape(D, 512)


def place_down(down_train):
    c = lax.axis_index("c")
    x = down_train.astype(BF).T
    keep, give = jnp.where(c == 0, x[:, :256], x[:, 256:]), jnp.where(c == 0, x[:, 256:], x[:, :256])
    x = by_core(c, keep, swap(give), 0)
    return lax.ppermute(x, FS_TP[:3], [(a * 16 + b, b * 16 + a) for a, b in EVERY])


def scatter_sum(hidden, down, ready):
    _, zl, c = (lax.axis_index(a) for a in TP)
    hidden = hidden.reshape(16, 2, 16, 256)
    across = (((1,), (1,)), ((), ()))
    keep, give = pick(hidden, c, 1).reshape(256, 256), pick(hidden, 1 - c, 1).reshape(256, 256)
    give = lax.dot_general(give, down, across, preferred_element_type=F32).astype(BF)
    got = swap(give)
    pair = lax.dot_general(keep, down, across, preferred_element_type=F32) + got.astype(F32)
    pair = pair.astype(BF).reshape(4, 4, 16, D)
    one, two, far = (pick(pair, (zl + d) & 3, 1) for d in (1 + 2 * c, 3 + 2 * c, 2))
    near = pick(pair, zl, 1).astype(F32)
    near += fan(one, 1).astype(F32) + fan(two, -1).astype(F32)
    one = fan(part_of(far, 2 * c, 2, 0), 2)
    two = fan(part_of(far, 2 - 2 * c, 2, 0), -2)
    far = by_core(c, one, two, 0)
    near, ready = lax.optimization_barrier(((near + far.astype(F32)).astype(BF), ready))
    rows = lax.all_to_all(near, "zh", 0, 0, tiled=True)
    return (*ready, jnp.sum(rows.astype(F32), axis=0).astype(BF))


def body(tokens, norm_gain, gate_train, up_train, down_train):
    gate_local = (norm_gain[:, None] * gate_train).astype(BF)
    up_local = (norm_gain[:, None] * up_train).astype(BF)
    both = spread(jnp.concatenate([gate_local, up_local], axis=1))
    down = spread(place_down(down_train))
    x = gather_tokens(tokens)
    wide = x.astype(F32)
    scale = lax.rsqrt(jnp.sum(wide * wide, axis=0) / D + EPS)[:, None]
    sums = lax.dot_general(x, both, (((0,), (0,)), ((), ())), preferred_element_type=F32)
    gate, up = sums[:, :256], sums[:, 256:]
    hidden = (jax.nn.silu(gate * scale) * (up * scale)).astype(BF)
    gate_serve, up_serve = both[:, :256], both[:, 256:]
    return scatter_sum(hidden, down, (gate_serve, up_serve, down.T))


def solution(mesh):
    finer = Mesh(mesh.devices.reshape(mesh.shape["fs"], 4, 4, 2), FS_TP)
    placed = (P("fs", TP), P("fs"), P("fs", TP), P("fs", TP), P("fs", TP))
    return jax.shard_map(
        body,
        mesh=finer,
        in_specs=placed,
        out_specs=(P(None, TP), P(None, TP), P(TP, None), P(FS_TP, None)),
        check_vma=False,
    )
```

```python
import jax
import jax.numpy as jnp
from jax import lax
from jax.experimental.layout import Layout, with_layout_constraint
from jax.sharding import Mesh
from jax.sharding import PartitionSpec as P


D = 2048
TP = ("zh", "zl", "c")
FS_TP = ("fs", "zh", "zl", "c")
EPS = 1e-06
SCALE = 2.0**13
WEIGHT_SCALE = 2.0**18
BF = jnp.bfloat16
F32 = jnp.float32
EVERY = [(a, b) for a in range(16) for b in range(16)]


def pick(x, i, dim):
    return lax.dynamic_index_in_dim(x, i, dim, keepdims=False, allow_negative_indices=False)


def part_of(x, at, size, dim):
    return lax.dynamic_slice_in_dim(x, at, size, dim, allow_negative_indices=False)


def fan(x, by):
    pairs = [(2 * z + c, 2 * ((z + (by, -by)[c]) % 16) + c) for z in range(16) for c in range(2)]
    return lax.ppermute(x, TP, pairs)


def swap(x):
    return lax.ppermute(x, "c", [(0, 1), (1, 0)])


def by_core(c, mine, other, dim):
    return jnp.concatenate([jnp.where(c == 0, mine, other), jnp.where(c == 0, other, mine)], axis=dim)


def row_major(x):
    return with_layout_constraint(x, Layout(major_to_minor=tuple(range(x.ndim))))


def packed(x, scale):
    return (x.astype(F32) * scale).astype(jnp.float16)


def unpacked(x, scale):
    return (x.astype(F32) / scale).astype(BF)


def gather_tokens(x):
    c = lax.axis_index("c")
    mine = lax.all_gather(x, TP[:2])[:, None]
    mine = lax.optimization_barrier(unpacked(mine, SCALE))
    other = swap(mine)
    return by_core(c, mine, other, 1).reshape(D, 512)


def place_down(down_train):
    c = lax.axis_index("c")
    x = down_train.astype(BF).T
    keep, give = jnp.where(c == 0, x[:, :256], x[:, 256:]), jnp.where(c == 0, x[:, 256:], x[:, :256])
    x = by_core(c, keep, swap(give), 0)
    return lax.ppermute(x, FS_TP[:3], [(a * 16 + b, b * 16 + a) for a, b in EVERY])


def scatter_sum(hidden, down, ready):
    _, zl, c = (lax.axis_index(a) for a in TP)
    hidden = hidden.reshape(16, 2, 16, 256)
    across = (((1,), (1,)), ((), ()))
    keep, give = pick(hidden, c, 1).reshape(256, 256), pick(hidden, 1 - c, 1).reshape(256, 256)
    give = lax.dot_general(give, down, across, preferred_element_type=F32).astype(BF)
    got = swap(give)
    pair = lax.dot_general(keep, down, across, preferred_element_type=F32) + got.astype(F32)
    pair = pair.astype(BF).reshape(4, 4, 16, D)
    one, two, far = (pick(pair, (zl + d) & 3, 1) for d in (1 + 2 * c, 3 + 2 * c, 2))
    near = pick(pair, zl, 1).astype(F32)
    near += fan(one, 1).astype(F32) + fan(two, -1).astype(F32)
    one = fan(part_of(far, 2 * c, 2, 0), 2)
    two = fan(part_of(far, 2 - 2 * c, 2, 0), -2)
    far = by_core(c, one, two, 0)
    near, ready = lax.optimization_barrier(((near + far.astype(F32)).astype(BF), ready))
    rows = lax.all_to_all(near, "zh", 0, 0, tiled=True)
    return (*ready, jnp.sum(rows.astype(F32), axis=0).astype(BF))


def body(tokens, norm_gain, gate_train, up_train, down_train):
    gate_local = (norm_gain[:, None] * gate_train).astype(BF)
    up_local = (norm_gain[:, None] * up_train).astype(BF)
    local = packed(jnp.concatenate([gate_local, up_local], axis=1), WEIGHT_SCALE)
    x, local = lax.optimization_barrier((packed(tokens.T, SCALE), local))
    local = jnp.concatenate([local, packed(place_down(down_train), WEIGHT_SCALE)], axis=1)
    every = row_major(lax.all_gather(row_major(local), "fs", tiled=True))
    both = unpacked(every[:, :512], WEIGHT_SCALE)
    down = row_major(unpacked(every[:, 512:], WEIGHT_SCALE))
    x = gather_tokens(x)
    wide = x.astype(F32)
    scale = lax.rsqrt(jnp.sum(wide * wide, axis=0) / D + EPS)[:, None]
    sums = lax.dot_general(x, both, (((0,), (0,)), ((), ())), preferred_element_type=F32)
    gate, up = sums[:, :256], sums[:, 256:]
    hidden = (jax.nn.silu(gate * scale) * (up * scale)).astype(BF)
    gate_serve, up_serve = both[:, :256], both[:, 256:]
    return scatter_sum(hidden, down, (gate_serve, up_serve, row_major(down.T)))


def solution(mesh):
    finer = Mesh(mesh.devices.reshape(mesh.shape["fs"], 4, 4, 2), FS_TP)
    placed = (P("fs", TP), P("fs"), P("fs", TP), P("fs", TP), P("fs", TP))
    return jax.shard_map(
        body,
        mesh=finer,
        in_specs=placed,
        out_specs=(P(None, TP), P(None, TP), P(TP, None), P(FS_TP, None)),
        check_vma=False,
    )
```

```python
import jax
import jax.numpy as jnp
from jax import lax
from jax.experimental.layout import Layout, with_layout_constraint
from jax.sharding import Mesh
from jax.sharding import PartitionSpec as P


D = 2048
TP = ("zh", "zl", "c")
FS_TP = ("fs", "zh", "zl", "c")
EPS = 1e-06
SCALE = 8192.0
BF = jnp.bfloat16
F32 = jnp.float32
EVERY = [(a, b) for a in range(16) for b in range(16)]


def pick(x, i, dim):
    return lax.dynamic_index_in_dim(x, i, dim, keepdims=False, allow_negative_indices=False)


def part_of(x, at, size, dim):
    return lax.dynamic_slice_in_dim(x, at, size, dim, allow_negative_indices=False)


def fan(x, by):
    pairs = [(2 * z + c, 2 * ((z + (by, -by)[c]) % 16) + c) for z in range(16) for c in range(2)]
    return lax.ppermute(x, TP, pairs)


def swap(x):
    return lax.ppermute(x, "c", [(0, 1), (1, 0)])


def by_core(c, mine, other, dim):
    return jnp.concatenate([jnp.where(c == 0, mine, other), jnp.where(c == 0, other, mine)], axis=dim)


def row_major(x):
    return with_layout_constraint(x, Layout(major_to_minor=tuple(range(x.ndim))))


def copies(x):
    return row_major(jnp.broadcast_to(x, (16, *x.shape)))


def spread(every):
    return row_major(lax.all_to_all(every, "fs", 0, 0, tiled=True)).reshape(D, every.shape[2])


def gather_tokens(x):
    c = lax.axis_index("c")
    mine = lax.all_gather(x, TP[:2])[:, None]
    mine = lax.optimization_barrier((mine.astype(F32) / SCALE).astype(BF))
    other = swap(mine)
    return by_core(c, mine, other, 1).reshape(D, 512)


def place_down(down_train):
    c = lax.axis_index("c")
    x = down_train.astype(BF).T
    keep, give = jnp.where(c == 0, x[:, :256], x[:, 256:]), jnp.where(c == 0, x[:, 256:], x[:, :256])
    x = by_core(c, keep, swap(give), 0)
    return lax.ppermute(x, FS_TP[:3], [(a * 16 + b, b * 16 + a) for a, b in EVERY])


def scatter_sum(hidden, down, ready):
    _, zl, c = (lax.axis_index(a) for a in TP)
    hidden = hidden.reshape(16, 2, 16, 256)
    across = (((1,), (1,)), ((), ()))
    keep, give = pick(hidden, c, 1).reshape(256, 256), pick(hidden, 1 - c, 1).reshape(256, 256)
    give = lax.dot_general(give, down, across, preferred_element_type=F32).astype(BF)
    got = swap(give)
    pair = lax.dot_general(keep, down, across, preferred_element_type=F32) + got.astype(F32)
    pair = pair.astype(BF).reshape(4, 4, 16, D)
    one, two, far = (pick(pair, (zl + d) & 3, 1) for d in (1 + 2 * c, 3 + 2 * c, 2))
    near = pick(pair, zl, 1).astype(F32)
    near += fan(one, 1).astype(F32) + fan(two, -1).astype(F32)
    one = fan(part_of(far, 2 * c, 2, 0), 2)
    two = fan(part_of(far, 2 - 2 * c, 2, 0), -2)
    far = by_core(c, one, two, 0)
    near, ready = lax.optimization_barrier(((near + far.astype(F32)).astype(BF), ready))
    rows = lax.all_to_all(near, "zh", 0, 0, tiled=True)
    return (*ready, jnp.sum(rows.astype(F32), axis=0).astype(BF))


def body(tokens, norm_gain, gate_train, up_train, down_train):
    gate_local = (norm_gain[:, None] * gate_train).astype(BF)
    up_local = (norm_gain[:, None] * up_train).astype(BF)
    both = spread(copies(jnp.concatenate([gate_local, up_local], axis=1)))
    x = (tokens.T.astype(F32) * SCALE).astype(jnp.float16)
    x, placed = lax.optimization_barrier((x, copies(place_down(down_train))))
    down = spread(placed)
    x = gather_tokens(x)
    wide = x.astype(F32)
    scale = lax.rsqrt(jnp.sum(wide * wide, axis=0) / D + EPS)[:, None]
    sums = lax.dot_general(x, both, (((0,), (0,)), ((), ())), preferred_element_type=F32)
    gate, up = sums[:, :256], sums[:, 256:]
    hidden = (jax.nn.silu(gate * scale) * (up * scale)).astype(BF)
    gate_serve, up_serve = both[:, :256], both[:, 256:]
    return scatter_sum(hidden, down, (gate_serve, up_serve, down.T))


def solution(mesh):
    finer = Mesh(mesh.devices.reshape(mesh.shape["fs"], 4, 4, 2), FS_TP)
    placed = (P("fs", TP), P("fs"), P("fs", TP), P("fs", TP), P("fs", TP))
    return jax.shard_map(
        body,
        mesh=finer,
        in_specs=placed,
        out_specs=(P(None, TP), P(None, TP), P(TP, None), P(FS_TP, None)),
        check_vma=False,
    )
```

```python
import jax
import jax.numpy as jnp
from jax import lax
from jax.experimental.layout import Layout, with_layout_constraint
from jax.sharding import Mesh
from jax.sharding import PartitionSpec as P


D = 2048
TP = ("zh", "zl", "c")
FS_TP = ("fs", "zh", "zl", "c")
EPS = 1e-06
SCALE = 8192.0
BF = jnp.bfloat16
F32 = jnp.float32
EVERY = [(a, b) for a in range(16) for b in range(16)]


def pick(x, i, dim):
    return lax.dynamic_index_in_dim(x, i, dim, keepdims=False, allow_negative_indices=False)


def part_of(x, at, size, dim):
    return lax.dynamic_slice_in_dim(x, at, size, dim, allow_negative_indices=False)


def put(whole, part, at):
    return lax.dynamic_update_slice(whole, part, at, allow_negative_indices=False)


def fan(x, by):
    pairs = [(2 * z + c, 2 * ((z + (by, -by)[c]) % 16) + c) for z in range(16) for c in range(2)]
    return lax.ppermute(x, TP, pairs)


def swap(x):
    return lax.ppermute(x, "c", [(0, 1), (1, 0)])


def row_major(x):
    return with_layout_constraint(x, Layout(major_to_minor=tuple(range(x.ndim))))


def spread(x):
    every = row_major(jnp.broadcast_to(x, (16, *x.shape)))
    return row_major(lax.all_to_all(every, "fs", 0, 0, tiled=True)).reshape(D, x.shape[1])


def gather_tokens(tokens):
    c = lax.axis_index("c")
    x = (tokens.T.astype(F32) * SCALE).astype(jnp.float16)
    mine = lax.all_gather(x, TP[:2])[:, None]
    mine = lax.optimization_barrier((mine.astype(F32) / SCALE).astype(BF))
    other = swap(mine)
    whole = put(jnp.zeros((16, 2, 64, 512), BF), mine, (0, c, 0, 0))
    return put(whole, other, (0, 1 - c, 0, 0)).reshape(D, 512)


def gather_down(down_train):
    x = down_train.astype(BF).T
    x = lax.ppermute(x, FS_TP[:3], [(a * 16 + b, b * 16 + a) for a, b in EVERY])
    x = jnp.broadcast_to(jnp.stack([x[:, :256], x[:, 256:]]), (16, 2, 64, 256)).reshape(32, 64, 256)
    return row_major(lax.all_to_all(row_major(x), ("fs", "c"), 0, 0, tiled=True)).reshape(D, 256)


def scatter_sum(hidden, down, ready):
    _, zl, c = (lax.axis_index(a) for a in TP)
    hidden = hidden.reshape(16, 2, 16, 256)
    across = (((1,), (1,)), ((), ()))
    keep, give = pick(hidden, c, 1).reshape(256, 256), pick(hidden, 1 - c, 1).reshape(256, 256)
    give = lax.dot_general(give, down, across, preferred_element_type=F32).astype(BF)
    got = swap(give)
    pair = lax.dot_general(keep, down, across, preferred_element_type=F32) + got.astype(F32)
    pair = pair.astype(BF).reshape(4, 4, 16, D)
    one, two, far = (pick(pair, (zl + d) & 3, 1) for d in (1 + 2 * c, 3 + 2 * c, 2))
    near = pick(pair, zl, 1).astype(F32)
    near += fan(one, 1).astype(F32) + fan(two, -1).astype(F32)
    one = fan(part_of(far, 2 * c, 2, 0), 2)
    two = fan(part_of(far, 2 - 2 * c, 2, 0), -2)
    half = lax.broadcasted_iota(jnp.int32, (2, 1, 1, 1), 0)
    far = jnp.where(half == c, one[None], two[None]).reshape(4, 16, D)
    near, ready = lax.optimization_barrier(((near + far.astype(F32)).astype(BF), ready))
    rows = lax.all_to_all(near, "zh", 0, 0, tiled=True)
    return (*ready, jnp.sum(rows.astype(F32), axis=0).astype(BF))


def body(tokens, norm_gain, gate_train, up_train, down_train):
    gate_local = (norm_gain[:, None] * gate_train).astype(BF)
    up_local = (norm_gain[:, None] * up_train).astype(BF)
    both = spread(jnp.concatenate([gate_local, up_local], axis=1))
    down = gather_down(down_train)
    x = gather_tokens(tokens)
    wide = x.astype(F32)
    scale = lax.rsqrt(jnp.sum(wide * wide, axis=0) / D + EPS)[:, None]
    sums = lax.dot_general(x, both, (((0,), (0,)), ((), ())), preferred_element_type=F32)
    gate, up = sums[:, :256], sums[:, 256:]
    hidden = (jax.nn.silu(gate * scale) * (up * scale)).astype(BF)
    gate_serve, up_serve = both[:, :256], both[:, 256:]
    return scatter_sum(hidden, down, (gate_serve, up_serve, down.T))


def solution(mesh):
    finer = Mesh(mesh.devices.reshape(mesh.shape["fs"], 4, 4, 2), FS_TP)
    placed = (P("fs", TP), P("fs"), P("fs", TP), P("fs", TP), P("fs", TP))
    return jax.shard_map(
        body,
        mesh=finer,
        in_specs=placed,
        out_specs=(P(None, TP), P(None, TP), P(TP, None), P(FS_TP, None)),
        check_vma=False,
    )
```

```python
import jax
import jax.numpy as jnp
from jax import lax
from jax.experimental.layout import Layout, with_layout_constraint
from jax.sharding import Mesh
from jax.sharding import PartitionSpec as P


D = 2048
TP = ("zh", "zl", "c")
FS_TP = ("fs", "zh", "zl", "c")
EPS = 1e-06
SCALE = 8192.0
BF = jnp.bfloat16
F32 = jnp.float32
EVERY = [(a, b) for a in range(16) for b in range(16)]


def pick(x, i, dim):
    return lax.dynamic_index_in_dim(x, i, dim, keepdims=False, allow_negative_indices=False)


def part_of(x, at, size, dim):
    return lax.dynamic_slice_in_dim(x, at, size, dim, allow_negative_indices=False)


def put(whole, part, at):
    return lax.dynamic_update_slice(whole, part, at, allow_negative_indices=False)


def fan(x, by):
    pairs = [(2 * z + c, 2 * ((z + (by, -by)[c]) % 16) + c) for z in range(16) for c in range(2)]
    return lax.ppermute(x, TP, pairs)


def swap(x):
    return lax.ppermute(x, "c", [(0, 1), (1, 0)])


def by_core(c, mine, other, dim):
    return jnp.concatenate([jnp.where(c == 0, mine, other), jnp.where(c == 0, other, mine)], axis=dim)


def row_major(x):
    return with_layout_constraint(x, Layout(major_to_minor=tuple(range(x.ndim))))


def spread(x):
    every = row_major(jnp.broadcast_to(x, (16, *x.shape)))
    return row_major(lax.all_to_all(every, "fs", 0, 0, tiled=True)).reshape(D, x.shape[1])


def gather_tokens(tokens):
    c = lax.axis_index("c")
    x = (tokens.T.astype(F32) * SCALE).astype(jnp.float16)
    mine = lax.all_gather(x, TP[:2])[:, None]
    mine = lax.optimization_barrier((mine.astype(F32) / SCALE).astype(BF))
    other = swap(mine)
    whole = put(jnp.zeros((16, 2, 64, 512), BF), mine, (0, c, 0, 0))
    return put(whole, other, (0, 1 - c, 0, 0)).reshape(D, 512)


def place_down(down_train):
    c = lax.axis_index("c")
    x = down_train.astype(BF).T
    keep, give = jnp.where(c == 0, x[:, :256], x[:, 256:]), jnp.where(c == 0, x[:, 256:], x[:, :256])
    x = by_core(c, keep, swap(give), 0)
    return lax.ppermute(x, FS_TP[:3], [(a * 16 + b, b * 16 + a) for a, b in EVERY])


def scatter_sum(hidden, down, ready):
    _, zl, c = (lax.axis_index(a) for a in TP)
    hidden = hidden.reshape(16, 2, 16, 256)
    across = (((1,), (1,)), ((), ()))
    keep, give = pick(hidden, c, 1).reshape(256, 256), pick(hidden, 1 - c, 1).reshape(256, 256)
    give = lax.dot_general(give, down, across, preferred_element_type=F32).astype(BF)
    got = swap(give)
    pair = lax.dot_general(keep, down, across, preferred_element_type=F32) + got.astype(F32)
    pair = pair.astype(BF).reshape(4, 4, 16, D)
    one, two, far = (pick(pair, (zl + d) & 3, 1) for d in (1 + 2 * c, 3 + 2 * c, 2))
    near = pick(pair, zl, 1).astype(F32)
    near += fan(one, 1).astype(F32) + fan(two, -1).astype(F32)
    one = fan(part_of(far, 2 * c, 2, 0), 2)
    two = fan(part_of(far, 2 - 2 * c, 2, 0), -2)
    half = lax.broadcasted_iota(jnp.int32, (2, 1, 1, 1), 0)
    far = jnp.where(half == c, one[None], two[None]).reshape(4, 16, D)
    near, ready = lax.optimization_barrier(((near + far.astype(F32)).astype(BF), ready))
    rows = lax.all_to_all(near, "zh", 0, 0, tiled=True)
    return (*ready, jnp.sum(rows.astype(F32), axis=0).astype(BF))


def body(tokens, norm_gain, gate_train, up_train, down_train):
    gate_local = (norm_gain[:, None] * gate_train).astype(BF)
    up_local = (norm_gain[:, None] * up_train).astype(BF)
    both = spread(jnp.concatenate([gate_local, up_local], axis=1))
    down = spread(place_down(down_train))
    x = gather_tokens(tokens)
    wide = x.astype(F32)
    scale = lax.rsqrt(jnp.sum(wide * wide, axis=0) / D + EPS)[:, None]
    sums = lax.dot_general(x, both, (((0,), (0,)), ((), ())), preferred_element_type=F32)
    gate, up = sums[:, :256], sums[:, 256:]
    hidden = (jax.nn.silu(gate * scale) * (up * scale)).astype(BF)
    gate_serve, up_serve = both[:, :256], both[:, 256:]
    return scatter_sum(hidden, down, (gate_serve, up_serve, down.T))


def solution(mesh):
    finer = Mesh(mesh.devices.reshape(mesh.shape["fs"], 4, 4, 2), FS_TP)
    placed = (P("fs", TP), P("fs"), P("fs", TP), P("fs", TP), P("fs", TP))
    return jax.shard_map(
        body,
        mesh=finer,
        in_specs=placed,
        out_specs=(P(None, TP), P(None, TP), P(TP, None), P(FS_TP, None)),
        check_vma=False,
    )
```
